32 devices in a mesh: sp: 8 (over z, x), tp: 4 (over y, core).
Axes of the slice: x: 2, y: 2, z: 4, core: 2. Of those that a mesh axis runs over, the one named last changes fastest.
Arguments:
- residual: bfloat16 [4096, 2048], P(('sp', 'tp')), may hold values from -6 to 6
- query_small: bfloat16 [4096, 8, 128], P('sp', 'tp'), may hold values from -120 to 120
- key_small: bfloat16 [4096, 8, 128], P('sp', 'tp'), may hold values from -6 to 6
- value_small: bfloat16 [4096, 8, 128], P('sp', 'tp'), may hold values from -6 to 6
- query_large: bfloat16 [4096, 8, 256], P('sp', 'tp'), may hold values from -120 to 120
- key_large: bfloat16 [4096, 8, 256], P('sp', 'tp'), may hold values from -6 to 6
- value_large: bfloat16 [4096, 8, 128], P('sp', 'tp'), may hold values from -6 to 6
- lambda_small: float32 [8], P('tp'), may hold values from 0.3 to 0.8
- lambda_large: float32 [8], P('tp'), may hold values from 0.3 to 0.8
- head_gain: float32 [128], replicated, may hold values from 0.1 to 1.9
- output_small: bfloat16 [1024, 2048], P('tp'), may hold values from -0.125 to 0.125
- output_large: bfloat16 [1024, 2048], P('tp'), may hold values from -0.125 to 0.125
- norm_gain: float32 [2048], replicated, may hold values from 0.1 to 1.9
- gate_weight: bfloat16 [2048, 5632], P('sp', 'tp'), may hold values from -0.125 to 0.125
- up_weight: bfloat16 [2048, 5632], P('sp', 'tp'), may hold values from -0.125 to 0.125
- down_weight: bfloat16 [5632, 2048], P('tp', 'sp'), may hold values from -0.3125 to 0.3125
Outputs:
- block_output: bfloat16 [4096, 2048], P(('sp', 'tp'))
The draws below stay inside these ranges and needn't reach their ends.
All inputs are finite; a program needn't handle non-finite values.
Results may differ from the reference program's by a relative error of at most 0.015.
Values may be sent and summed in bfloat16 or wider, within the bound.
No kernel may reach another device: no remote copies, remote signals or barrier semaphores. Data moves between devices by JAX's collectives and lax.ppermute only.
A program may use at most 128 MiB of HBM per device.

```python
import math
import jax
import jax.numpy as jnp
from jax import lax

D = 2048
HA = 8
HB = 8
KA = 64
KB = 128
VD = 128
FF = 5632
SEQ = 4096


def draw_pair(key, head_count, width, salt):
    base = jax.random.fold_in(key, salt)
    key_draw, query_draw = jax.random.split(base, 2)
    key_rows = jnp.clip(1.3 * jax.random.normal(key_draw, (SEQ, head_count, width), jnp.float32), -6.0, 6.0)
    query_rows = jnp.clip(1.3 * jax.random.normal(query_draw, (SEQ, head_count, width), jnp.float32), -6.0, 6.0)
    return (query_rows, key_rows)


def draw_query_small(key, part):
    return draw_pair(key, HA, 2 * KA, 11)[0].astype(jnp.bfloat16)


def draw_key_small(key, part):
    return draw_pair(key, HA, 2 * KA, 11)[1].astype(jnp.bfloat16)


def draw_query_large(key, part):
    return draw_pair(key, HB, 2 * KB, 23)[0].astype(jnp.bfloat16)


def draw_key_large(key, part):
    return draw_pair(key, HB, 2 * KB, 23)[1].astype(jnp.bfloat16)


def block_levels(key, shape, shards, least, largest):
    def one(position, blocks):
        heights = jax.random.uniform(jax.random.fold_in(jax.random.fold_in(key, 6), position), (blocks,), jnp.float32, least / len(shards), largest / len(shards))
        return jnp.repeat(jnp.exp(heights), shape[position] // blocks).reshape((-1,) + (1,) * (len(shape) - position - 1))

    factor_of = one(*shards[0])
    for cut in shards[1:]:
        factor_of = factor_of * one(*cut)
    return factor_of


def scatter_about(key, shape, scale, bound, shards=(), kind=jnp.bfloat16):
    values = jax.random.normal(key, shape, jnp.float32) * scale
    if len(shards) > 0:
        values = block_levels(key, shape, shards, -0.22, 0.18) * values
    return jnp.clip(values, min=-bound, max=bound).astype(kind)


def setup_inputs(seed: int = 0) -> dict:
    key_list = jax.random.split(jax.random.key(seed), 17)
    return {
        "residual": scatter_about(key_list[0], (SEQ, D), 1.0, 6.0, ((0, 32),)),
        "query_small": draw_query_small(jax.random.fold_in(key_list[16], 71), 0),
        "key_small": draw_key_small(jax.random.fold_in(key_list[16], 71), 0),
        "value_small": scatter_about(key_list[3], (SEQ, HA, VD), 1.0, 6.0, ((0, 8), (1, 4))),
        "query_large": draw_query_large(jax.random.fold_in(key_list[16], 71), 0),
        "key_large": draw_key_large(jax.random.fold_in(key_list[16], 71), 0),
        "value_large": scatter_about(key_list[6], (SEQ, HB, VD), 1.0, 6.0, ((0, 8), (1, 4))),
        "lambda_small": jnp.clip(0.3 + 0.5 * jax.random.uniform(key_list[7], (HA,), jnp.float32) ** block_levels(key_list[7], (HA,), ((0, 4),), -0.2, 0.2), 0.3, 0.8),
        "lambda_large": jnp.clip(0.3 + 0.5 * jax.random.uniform(key_list[8], (HB,), jnp.float32) ** block_levels(key_list[8], (HB,), ((0, 4),), -0.2, 0.2), 0.3, 0.8),
        "head_gain": jnp.clip(1.0 + 0.18 * jax.random.normal(key_list[9], (VD,), jnp.float32), 0.1, 1.9),
        "output_small": scatter_about(key_list[10], (HA * VD, D), ((HA + HB) * VD) ** -0.5, 0.125, ((0, 4),)),
        "output_large": scatter_about(key_list[11], (HB * VD, D), ((HA + HB) * VD) ** -0.5, 0.125, ((0, 4),)),
        "norm_gain": jnp.clip(1.0 + 0.18 * jax.random.normal(key_list[12], (D,), jnp.float32), 0.1, 1.9),
        "gate_weight": scatter_about(key_list[13], (D, FF), D ** -0.5, 0.125, ((0, 8), (1, 4))),
        "up_weight": scatter_about(key_list[14], (D, FF), D ** -0.5, 0.125, ((0, 8), (1, 4))),
        "down_weight": scatter_about(key_list[15], (FF, D), (FF // 16) ** -0.5, 0.3125, ((0, 4), (1, 8))),
    }


residual_scale = 8.0 ** 0.25
branch_scale = 0.8
norm_epsilon = 1e-05
masked_score = -1e+30

def head_group(queries, key_rows, values, lambdas, head_gain):
    length, head_count, doubled = queries.shape
    head_size = doubled // 2
    score_scale = head_size ** (-0.5)
    query_maps = queries.reshape(length, head_count, 2, head_size).astype(jnp.float32)
    key_maps = key_rows.reshape(length, head_count, 2, head_size).astype(jnp.float32)
    value_rows = values.astype(jnp.float32)
    block_size = math.gcd(length, 256)
    key_index = jnp.arange(length, dtype=jnp.int32)

    def one_block(block_index):
        offset = block_index * block_size
        query_block = lax.dynamic_slice_in_dim(query_maps, offset, block_size, 0)
        scores = jnp.einsum('qhmd,khmd->hmqk', query_block, key_maps) * score_scale
        query_index = offset + jnp.arange(block_size, dtype=jnp.int32)
        visible = key_index[None, :] <= query_index[:, None]
        scores = jnp.where(visible, scores, masked_score)
        highest = lax.optimization_barrier(jnp.max(scores, axis=-1, keepdims=True))
        weights = jnp.where(visible, jnp.exp(scores - highest), 0.0)
        totals = lax.optimization_barrier(jnp.sum(weights, axis=-1))
        rounded = lax.optimization_barrier(weights.astype(jnp.bfloat16)).astype(jnp.float32)
        map_out = jnp.einsum('hmqk,khe->hmqe', rounded, value_rows) / totals[..., None]
        combined = map_out[:, 0] - lambdas[:, None, None] * map_out[:, 1]
        mean_square = lax.optimization_barrier(jnp.mean(combined * combined, axis=-1, keepdims=True))
        normed = combined * lax.rsqrt(mean_square + norm_epsilon) * head_gain * branch_scale
        return jnp.transpose(normed, (1, 0, 2)).astype(jnp.bfloat16)
    blocks = lax.map(one_block, jnp.arange(length // block_size, dtype=jnp.int32))
    return blocks.reshape(length, head_count * values.shape[2])

def layer_norm(values, gains):
    centered = values - lax.optimization_barrier(jnp.mean(values, axis=-1, keepdims=True))
    variance = lax.optimization_barrier(jnp.mean(centered * centered, axis=-1, keepdims=True))
    return centered * lax.rsqrt(variance + norm_epsilon) * gains

def reference(residual, query_small, key_small, value_small, query_large, key_large, value_large, lambda_small, lambda_large, head_gain, output_small, output_large, norm_gain, gate_weight, up_weight, down_weight):
    attended_small = head_group(query_small, key_small, value_small, lambda_small, head_gain)
    attended_large = head_group(query_large, key_large, value_large, lambda_large, head_gain)
    mixed_sum = jnp.dot(attended_small, output_small, preferred_element_type=jnp.float32) + jnp.dot(attended_large, output_large, preferred_element_type=jnp.float32)
    pre_norm = residual_scale * residual.astype(jnp.float32) + mixed_sum
    normed = layer_norm(pre_norm, norm_gain).astype(jnp.bfloat16)
    gate_rows = jnp.dot(normed, gate_weight, preferred_element_type=jnp.float32)
    up_rows = jnp.dot(normed, up_weight, preferred_element_type=jnp.float32)
    hidden = (jax.nn.silu(gate_rows) * up_rows).astype(jnp.bfloat16)
    down_sum = jnp.dot(hidden, down_weight, preferred_element_type=jnp.float32)
    return (residual_scale * normed.astype(jnp.float32) + 0.5 * down_sum).astype(jnp.bfloat16)
```

```python
import functools

import jax
import jax.numpy as jnp
from jax import lax
from jax.experimental import pallas as pl
from jax.experimental.pallas import tpu as pltpu
from jax.sharding import PartitionSpec as P

residual_scale = 8.0**0.25
branch_scale = 0.8
norm_epsilon = 1e-05
masked_score = -1e30
log2_e = 1.4426950408889634
bf16 = jnp.bfloat16
f32 = jnp.float32


NT = (((1,), (1,)), ((), ()))
vmem = pl.BlockSpec(memory_space=pltpu.VMEM)
smem = pl.BlockSpec(memory_space=pltpu.SMEM)
hbm = pl.BlockSpec(memory_space=pl.ANY)


def params(limit=60 << 20):
    return pltpu.CompilerParams(vmem_limit_bytes=limit)


def swap(value, axis, mask, allowed=None):
    size = lax.axis_size(axis)
    pairs = [(i, i ^ mask) for i in range(size) if allowed is None or allowed(i, i ^ mask)]
    return lax.ppermute(value, axis, pairs)


def attention_kernel(
    index_ref, lam_ref, gain_ref, *refs, widths, query_count, half_count, tile, chunk
):
    w = widths
    vw = refs[half_count * 2].shape[1]
    own = refs[:half_count]
    cross = refs[half_count : 2 * half_count]
    outs = refs[2 * half_count : 2 * half_count + query_count]
    q_buf, k_buf, v_buf, acc, peak, sems = refs[2 * half_count + query_count :]
    s = index_ref[0]
    upper = s >= half_count
    local = s % half_count
    copies = []
    for e in range(half_count):
        place = s ^ e
        width = own[e].shape[1]
        base = width - 2 * w - vw
        if e < query_count:
            copies.append(pltpu.make_async_copy(own[e].at[:, 0 : 2 * w], q_buf.at[e], sems.at[0]))
        copies.append(
            pltpu.make_async_copy(own[e].at[:, base : base + 2 * w], k_buf.at[place], sems.at[0])
        )
        copies.append(
            pltpu.make_async_copy(
                own[e].at[:, base + 2 * w :], v_buf.at[place, :, 0:vw], sems.at[0]
            )
        )
    for c in copies:
        c.start()

    def cross_copies():
        items = []
        for e in range(half_count):
            place = local ^ e
            items.append(
                pltpu.make_async_copy(cross[e].at[:, 0 : 2 * w], k_buf.at[place], sems.at[1])
            )
            items.append(
                pltpu.make_async_copy(
                    cross[e].at[:, 2 * w :], v_buf.at[place, :, 0:vw], sems.at[1]
                )
            )
        return items

    @pl.when(upper)
    def _():
        for c in cross_copies():
            c.start()

    for b in range(2 * half_count):
        v_buf[b, :, vw:] = jnp.ones((chunk, v_buf.shape[2] - vw), bf16)
    for c in copies:
        c.wait()

    @pl.when(upper)
    def _():
        for c in cross_copies():
            c.wait()

    scale = w**-0.5 * log2_e
    lam = lam_ref[0]
    tiles = chunk // tile

    for e in range(query_count):
        place = s ^ e

        def one_tile(i, carry):
            row = pl.multiple_of(i * tile, tile)
            acc[...] = jnp.zeros_like(acc)
            peak[...] = jnp.full_like(peak, masked_score)

            def block(j, masked):
                for m in range(2):
                    q = q_buf[e, pl.ds(row, tile), m * w : (m + 1) * w]
                    k = k_buf[j, :, m * w : (m + 1) * w]
                    scores = lax.dot_general(q, k, NT, preferred_element_type=f32)
                    if masked:
                        qi = row + lax.broadcasted_iota(jnp.int32, (tile, chunk), 0)
                        ki = lax.broadcasted_iota(jnp.int32, (tile, chunk), 1)
                        scores = jnp.where(ki <= qi, scores, masked_score)
                    old = peak[m, :, 0:1]
                    new = jnp.maximum(old, jnp.max(scores, axis=-1, keepdims=True))
                    fade = jnp.exp2((old - new) * scale)
                    weights = jnp.exp2((scores - new) * scale).astype(bf16)
                    part = jnp.dot(weights, v_buf[j], preferred_element_type=f32)
                    acc[m] = acc[m] * fade + part
                    peak[m] = jnp.broadcast_to(new, peak.shape[1:])

            def body(j, c):
                block(j, False)
                return c

            lax.fori_loop(0, place, body, 0)
            block(place, True)
            one = acc[0, :, 0:vw] / acc[0, :, vw : vw + 1]
            two = acc[1, :, 0:vw] / acc[1, :, vw : vw + 1]
            combined = one - lam * two
            square = jnp.mean(combined * combined, axis=-1, keepdims=True)
            result = combined * lax.rsqrt(square + norm_epsilon) * gain_ref[...] * branch_scale
            outs[e][pl.ds(row, tile), :] = result.astype(bf16)
            return carry

        lax.fori_loop(0, tiles, one_tile, 0)


def attention(index, lam, gain, own, cross, w, query_count):
    half_count = len(own)
    chunk = own[0].shape[0]
    vw = gain.shape[1]
    tile = min(256, chunk)
    return pl.pallas_call(
        functools.partial(
            attention_kernel,
            widths=w,
            query_count=query_count,
            half_count=half_count,
            tile=tile,
            chunk=chunk,
        ),
        out_shape=[jax.ShapeDtypeStruct((chunk, vw), bf16)] * query_count,
        in_specs=[smem, smem, vmem] + [hbm] * (2 * half_count),
        out_specs=[vmem] * query_count,
        scratch_shapes=[
            pltpu.VMEM((query_count, chunk, 2 * w), bf16),
            pltpu.VMEM((2 * half_count, chunk, 2 * w), bf16),
            pltpu.VMEM((2 * half_count, chunk, 2 * vw), bf16),
            pltpu.VMEM((2, tile, 2 * vw), f32),
            pltpu.VMEM((2, tile, 128), f32),
            pltpu.SemaphoreType.DMA((2,)),
        ],
        compiler_params=params(),
        name=f"attention_{w}",
    )(index, lam, gain, *own, *cross)


def project_kernel(index_ref, w_ref, *refs, heads, y_count, c_count, rows):
    att = refs[:heads]
    keep_ref, send_ref = refs[heads : heads + 2]
    first = index_ref[0]
    y = index_ref[1]
    c = index_ref[2]
    vw = att[0].shape[1]
    weight = jnp.concatenate(
        [w_ref[pl.ds(pl.multiple_of((first ^ e) * vw, vw), vw), :] for e in range(heads)], axis=0
    )
    for which, out in ((0, keep_ref), (1, send_ref)):
        blocks = []
        for e in range(y_count):
            start = pl.multiple_of(((y ^ e) * c_count + (c ^ which)) * rows, rows)
            blocks.append(
                jnp.concatenate([att[h][pl.ds(start, rows), :] for h in range(heads)], axis=1)
            )
        lhs = jnp.concatenate(blocks, axis=0)
        out[...] = jnp.dot(lhs, weight, preferred_element_type=f32).astype(out.dtype)


def norm_kernel(*refs, count):
    parts = refs[:count]
    residual_ref, gain_ref, out_ref = refs[count:]
    total = residual_scale * residual_ref[...].astype(f32)
    for p in parts:
        total = total + p[...].astype(f32)
    centered = total - jnp.mean(total, axis=-1, keepdims=True)
    variance = jnp.mean(centered * centered, axis=-1, keepdims=True)
    out_ref[...] = (centered * lax.rsqrt(variance + norm_epsilon) * gain_ref[...]).astype(bf16)


def hidden_kernel(index_ref, *refs, blocks, y_count, s_count, fp):
    rows_in = refs[:blocks]
    packs = refs[blocks : blocks + y_count * s_count]
    out_ref, rows, gate, up, sems = refs[blocks + y_count * s_count :]
    s = index_ref[0]
    n = rows_in[0].shape[0]
    copies = []
    for b in range(blocks):
        copies.append(
            pltpu.make_async_copy(rows_in[b], rows.at[pl.ds(b * n, n), :], sems.at[0])
        )
    for y in range(y_count):
        for m in range(s_count):
            pack = packs[y * s_count + m]
            place = s ^ m
            copies.append(
                pltpu.make_async_copy(
                    pack.at[pl.ds(0, fp), :], gate.at[place, pl.ds(y * fp, fp), :], sems.at[1]
                )
            )
            copies.append(
                pltpu.make_async_copy(
                    pack.at[pl.ds(fp, fp), :], up.at[place, pl.ds(y * fp, fp), :], sems.at[1]
                )
            )
    for c in copies:
        c.start()
    for c in copies:
        c.wait()
    total = blocks * n
    tile = min(512, total)

    def body(i, carry):
        at = pl.multiple_of(i * tile, tile)
        lhs = rows[pl.ds(at, tile), :]
        g = lax.dot_general(
            lhs,
            jnp.concatenate([gate[k] for k in range(s_count)], axis=1),
            NT,
            preferred_element_type=f32,
        )
        u = lax.dot_general(
            lhs,
            jnp.concatenate([up[k] for k in range(s_count)], axis=1),
            NT,
            preferred_element_type=f32,
        )
        out_ref[pl.ds(at, tile), :] = (g / (1.0 + jnp.exp(-g)) * u).astype(bf16)
        return carry

    lax.fori_loop(0, total // tile, body, 0)


def down_kernel(index_ref, h_ref, *refs, y_count, s_count, fp, groups):
    packs = refs[: y_count * s_count]
    outs = refs[y_count * s_count : y_count * s_count + groups]
    down, sems = refs[y_count * s_count + groups :]
    s = index_ref[0]
    copies = []
    for y in range(y_count):
        for m in range(s_count):
            copies.append(
                pltpu.make_async_copy(
                    packs[y * s_count + m].at[pl.ds(2 * fp, fp), :],
                    down.at[s ^ m, pl.ds(y * fp, fp), :],
                    sems.at[0],
                )
            )
    for c in copies:
        c.start()
    for c in copies:
        c.wait()
    width = down.shape[2]
    total = h_ref.shape[0]
    n = total // groups
    for k in range(s_count):
        for b in range(groups):
            part = jnp.dot(
                h_ref[b * n : (b + 1) * n, :], down[k], preferred_element_type=f32
            )
            outs[b][:, k * width : (k + 1) * width] = part.astype(outs[b].dtype)


def final_kernel(normed_ref, *refs):
    parts = refs[:-1]
    total = parts[0][...].astype(f32)
    for p in parts[1:]:
        total = total + p[...].astype(f32)
    refs[-1][...] = (residual_scale * normed_ref[...].astype(f32) + 0.5 * total).astype(bf16)


def per_device(
    residual,
    query_small,
    key_small,
    value_small,
    query_large,
    key_large,
    value_large,
    lambda_small,
    lambda_large,
    head_gain,
    output_small,
    output_large,
    norm_gain,
    gate_weight,
    up_weight,
    down_weight,
):
    s_count = lax.axis_size("sp")
    t_count = lax.axis_size("tp")
    half_count = s_count // 2
    c_count = 2
    y_count = t_count // c_count
    s = lax.axis_index("sp")
    t = lax.axis_index("tp")
    y = t // c_count
    c = t % c_count
    local = s % half_count
    chunk, small_heads, small_width = query_small.shape
    large_heads, large_width = query_large.shape[1:]
    heads = small_heads + large_heads
    vw = value_small.shape[2]
    own_rows, width = residual.shape
    role = local % heads
    is_large = role < large_heads

    def head_of(index):
        return index % heads

    def packed(q, k, v, count):
        both, only = [], []
        flip = local % count
        for e in range(count):
            picks = []
            for a in (q, k, v):
                pick = a[:, e]
                for other in range(count):
                    if other != e:
                        pick = jnp.where((flip ^ e) == other, a[:, other], pick)
                picks.append(pick)
            both.append(jnp.concatenate(picks, axis=1))
            only.append(jnp.concatenate(picks[1:], axis=1))
        return both, only

    large_both, large_only = packed(query_large, key_large, value_large, large_heads)
    small_both, small_only = packed(query_small, key_small, value_small, small_heads)

    def to_large(i, j):
        return head_of(j % half_count) < large_heads

    def to_small(i, j):
        return head_of(j % half_count) >= large_heads

    def upward(test):
        return lambda i, j: i < half_count <= j and test(i, j)

    own_large, own_small, cross_large, cross_small = [], [], [], []
    for e in range(half_count):
        source = (large_both, small_both) if e < heads else (large_only, small_only)
        if e == 0:
            own_large.append(source[0][0])
            own_small.append(source[1][0])
        else:
            own_large.append(swap(source[0][e % large_heads], "sp", e, to_large))
            own_small.append(swap(source[1][e % small_heads], "sp", e, to_small))
    for e in range(half_count):
        mask = half_count | e
        cross_large.append(swap(large_only[e % large_heads], "sp", mask, upward(to_large)))
        cross_small.append(swap(small_only[e % small_heads], "sp", mask, upward(to_small)))

    slice_width = gate_weight.shape[0]
    fb = gate_weight.shape[1] // half_count
    fp = -(-fb // 16) * 16

    def blocks_of(rows):
        rows = rows.reshape(half_count, fb, slice_width)
        return jnp.pad(rows, ((0, 0), (0, fp - fb), (0, 0))) if fp != fb else rows

    packs = jnp.concatenate(
        [blocks_of(gate_weight.T), blocks_of(up_weight.T), blocks_of(down_weight)], axis=1
    )
    by_offset = [
        lax.dynamic_index_in_dim(packs, local ^ e, 0, keepdims=False) for e in range(half_count)
    ]
    mine = [
        by_offset[m % half_count] if m == 0 else swap(by_offset[m % half_count], "sp", m)
        for m in range(s_count)
    ]
    all_packs = list(mine)
    for e in range(1, y_count):
        all_packs += [swap(p, "tp", e * c_count) for p in mine]

    index = s.astype(jnp.int32).reshape(1)
    lam_large = lambda_large[role % large_heads]
    lam_small = lambda_small[role % small_heads]
    gain = head_gain.reshape(1, vw)

    def take_large(operands):
        own, cross, _, _ = operands
        return attention(index, lam_large.reshape(1), gain, own, cross, large_width // 2, heads)

    def take_small(operands):
        _, _, own, cross = operands
        return attention(index, lam_small.reshape(1), gain, own, cross, small_width // 2, heads)

    results = lax.cond(
        is_large, take_large, take_small, (own_large, cross_large, own_small, cross_small)
    )
    attended = [results[0]] + [swap(results[e], "sp", e) for e in range(1, heads)]

    out_weight = jnp.concatenate([output_large, output_small], axis=0)
    where = jnp.stack([role, y, c]).astype(jnp.int32)
    part_rows = y_count * own_rows
    keep, send = pl.pallas_call(
        functools.partial(
            project_kernel, heads=heads, y_count=y_count, c_count=c_count, rows=own_rows
        ),
        out_shape=[
            jax.ShapeDtypeStruct((part_rows, width), f32),
            jax.ShapeDtypeStruct((part_rows, width), bf16),
        ],
        in_specs=[smem] + [vmem] * (1 + heads),
        out_specs=[vmem] * 2,
        compiler_params=params(),
        name="project",
    )(where, out_weight, *attended)
    other = swap(send, "tp", 1)
    mixed = keep + other.astype(f32)
    parts = [mixed[:own_rows]]
    for e in range(1, y_count):
        parts.append(
            swap(mixed[e * own_rows : (e + 1) * own_rows].astype(bf16), "tp", e * c_count)
        )
    normed = pl.pallas_call(
        functools.partial(norm_kernel, count=len(parts)),
        out_shape=jax.ShapeDtypeStruct((own_rows, width), bf16),
        compiler_params=params(),
        name="norm",
    )(*parts, residual, norm_gain.reshape(1, width))

    own_c = [normed] + [swap(normed, "sp", e) for e in range(1, half_count)]
    other_c = [swap(r, "tp", 1) for r in own_c]
    blocks = 2 * half_count
    hidden = pl.pallas_call(
        functools.partial(
            hidden_kernel, blocks=blocks, y_count=y_count, s_count=s_count, fp=fp
        ),
        out_shape=jax.ShapeDtypeStruct((blocks * own_rows, y_count * fp), bf16),
        in_specs=[smem] + [hbm] * (blocks + y_count * s_count),
        out_specs=vmem,
        scratch_shapes=[
            pltpu.VMEM((blocks * own_rows, width), bf16),
            pltpu.VMEM((s_count, y_count * fp, slice_width), bf16),
            pltpu.VMEM((s_count, y_count * fp, slice_width), bf16),
            pltpu.SemaphoreType.DMA((2,)),
        ],
        compiler_params=params(),
        name="hidden",
    )(index, *own_c, *other_c, *all_packs)
    groups = 2
    summed = pl.pallas_call(
        functools.partial(
            down_kernel, y_count=y_count, s_count=s_count, fp=fp, groups=groups
        ),
        out_shape=[
            jax.ShapeDtypeStruct((half_count * own_rows, width), f32),
            jax.ShapeDtypeStruct((half_count * own_rows, width), bf16),
        ],
        in_specs=[smem, vmem] + [hbm] * (y_count * s_count),
        out_specs=[vmem] * groups,
        scratch_shapes=[
            pltpu.VMEM((s_count, y_count * fp, slice_width), bf16),
            pltpu.SemaphoreType.DMA((1,)),
        ],
        compiler_params=params(),
        name="down",
    )(index, hidden, *all_packs)
    total = summed[0] + swap(summed[1], "tp", 1).astype(f32)
    finals = [total[:own_rows]]
    for e in range(1, half_count):
        finals.append(swap(total[e * own_rows : (e + 1) * own_rows].astype(bf16), "sp", e))
    return pl.pallas_call(
        final_kernel,
        out_shape=jax.ShapeDtypeStruct((own_rows, width), bf16),
        compiler_params=params(),
        name="final",
    )(normed, *finals)


def solution(mesh):
    in_specs = (
        P(("sp", "tp"), None),
        P("sp", "tp", None),
        P("sp", "tp", None),
        P("sp", "tp", None),
        P("sp", "tp", None),
        P("sp", "tp", None),
        P("sp", "tp", None),
        P("tp"),
        P("tp"),
        P(),
        P("tp", None),
        P("tp", None),
        P(),
        P("sp", "tp"),
        P("sp", "tp"),
        P("tp", "sp"),
    )
    out_specs = P(("sp", "tp"), None)
    return jax.shard_map(
        per_device, mesh=mesh, in_specs=in_specs, out_specs=out_specs, check_vma=False
    )
```
